32 devices in a mesh: sp: 16 (over z, y, x), tp: 2 (over core).
Axes of the slice: x: 2, y: 2, z: 4, core: 2. Of those that a mesh axis runs over, the one named last changes fastest.
Arguments:
- tokens: bfloat16 [4096, 2048], P('sp', 'tp'), may hold values from -12 to 12
- norm_gain: float32 [2048], replicated, may hold values from 0.1 to 1.9
- window_query: bfloat16 [2048, 1024], P(None, 'tp'), may hold values from -2 to 2
- window_key: bfloat16 [2048, 512], P(None, 'tp'), may hold values from -2 to 2
- window_value: bfloat16 [2048, 512], P(None, 'tp'), may hold values from -0.125 to 0.125
- window_gate: bfloat16 [2048, 1024], P(None, 'tp'), may hold values from -0.125 to 0.125
- window_sink: float32 [16], P('tp'), may hold values from 2 to 6
- pair_query: bfloat16 [2048, 1024], P(None, 'tp'), may hold values from -2 to 2
- pair_key: bfloat16 [2048, 1024], P(None, 'tp'), may hold values from -2 to 2
- pair_value: bfloat16 [2048, 1024], P(None, 'tp'), may hold values from -0.125 to 0.125
- pair_gate: bfloat16 [2048, 1024], P(None, 'tp'), may hold values from -0.125 to 0.125
- map_lambda: float32 [8], P('tp'), may hold values from 0.3 to 0.8
- head_gain: float32 [128], replicated, may hold values from 0.1 to 1.9
- window_out: bfloat16 [1024, 2048], P('tp'), may hold values from -0.125 to 0.125
- pair_out: bfloat16 [1024, 2048], P('tp'), may hold values from -0.125 to 0.125
Outputs:
- mixed: bfloat16 [4096, 2048], P(('sp', 'tp'))
The draws below stay inside these ranges and needn't reach their ends.
All inputs are finite; a program needn't handle non-finite values.
Results may differ from the reference program's by a relative error of at most 0.018.
Values may be sent and summed in bfloat16 or wider, within the bound.
A program may use at most 128 MiB of HBM per device.

```python
import math
import jax
import jax.numpy as jnp
from jax import lax

D = 2048
HD = 64
A_HEADS = 16
A_KV = 8
B_HEADS = 8
WINDOW = 128
SEQ = 4096
HEAD_GROUPS = 2


def base_weight(key, noise_tag, columns, fan_in):
    noise = jax.random.normal(jax.random.fold_in(key, noise_tag), (D, columns), jnp.float32)
    return jnp.clip(noise, -6.0, 6.0) * fan_in ** (-0.5)


def draw_tokens(key, part):
    values = jnp.clip(jax.random.normal(jax.random.fold_in(key, 21), (SEQ, D), jnp.float32), -6.0, 6.0)
    return values.astype(jnp.bfloat16)


def draw_window_query(key, part):
    weight = base_weight(key, 31, A_HEADS * HD, D)
    return weight.astype(jnp.bfloat16)


def draw_window_key(key, part):
    weight = base_weight(key, 32, A_KV * HD, D)
    return weight.astype(jnp.bfloat16)


def draw_pair_query(key, part):
    weight = base_weight(key, 33, B_HEADS * 2 * HD, D // 2)
    return weight.astype(jnp.bfloat16)


def draw_pair_key(key, part):
    weight = base_weight(key, 34, B_HEADS * 2 * HD, D // 2)
    return weight.astype(jnp.bfloat16)


def shard_levels(own_key, extent, pieces, least, top_value):
    def one(axis_at, parts):
        draws = jax.random.uniform(jax.random.fold_in(jax.random.fold_in(own_key, 6), axis_at), (parts,), jnp.float32, least / len(pieces), top_value / len(pieces))
        return jnp.repeat(jnp.exp(draws), extent[axis_at] // parts).reshape((-1,) + (1,) * (len(extent) - axis_at - 1))

    gain = one(*pieces[0])
    for cut in pieces[1:]:
        gain = gain * one(*cut)
    return gain


def gaussian(rng, shape, scale, bound, pieces=(), kind=jnp.bfloat16):
    loudness = shard_levels(rng, shape, pieces, -0.22, 0.18) if pieces else 1.0
    values = jax.random.normal(rng, shape, jnp.float32) * scale * loudness
    return jnp.minimum(jnp.maximum(values, -bound), bound).astype(kind)


def setup_inputs(seed: int = 0) -> dict:
    key_list = jax.random.split(jax.random.key(seed), 16)
    tokens = draw_tokens(jax.random.fold_in(key_list[15], 71), 0)
    norm_gain = jnp.clip(1.0 + 0.18 * jax.random.normal(key_list[1], (D,), jnp.float32), 0.1, 1.9)
    window_query = draw_window_query(jax.random.fold_in(key_list[15], 71), 0)
    window_key = draw_window_key(jax.random.fold_in(key_list[15], 71), 0)
    window_value = gaussian(key_list[4], (D, A_KV * HD), D ** -0.5, 0.125, ((1, 2),))
    window_gate = gaussian(key_list[5], (D, A_HEADS * HD), D ** -0.5, 0.125, ((1, 2),))
    window_sink = jnp.clip(2.0 + 4.0 * jax.random.uniform(key_list[6], (A_HEADS,), jnp.float32) ** shard_levels(key_list[6], (A_HEADS,), ((0, 2),), -0.2, 0.2), 2.0, 6.0)
    pair_query = draw_pair_query(jax.random.fold_in(key_list[15], 71), 0)
    pair_key = draw_pair_key(jax.random.fold_in(key_list[15], 71), 0)
    pair_value = gaussian(key_list[9], (D, B_HEADS * 2 * HD), D ** -0.5, 0.125, ((1, 2),))
    pair_gate = gaussian(key_list[10], (D, B_HEADS * 2 * HD), D ** -0.5, 0.125, ((1, 2),))
    map_lambda = jnp.clip(0.3 + 0.5 * jax.random.uniform(key_list[11], (B_HEADS,), jnp.float32) ** shard_levels(key_list[11], (B_HEADS,), ((0, 2),), -0.2, 0.2), 0.3, 0.8)
    head_gain = jnp.clip(1.0 + 0.18 * jax.random.normal(key_list[12], (2 * HD,), jnp.float32), 0.1, 1.9)
    window_out = gaussian(key_list[13], (A_HEADS * HD, D), (A_HEADS * HD + 2 * B_HEADS * HD) ** -0.5, 0.125, ((0, 2),))
    pair_out = gaussian(key_list[14], (2 * B_HEADS * HD, D), (A_HEADS * HD + 2 * B_HEADS * HD) ** -0.5, 0.125, ((0, 2),))
    return dict(tokens=tokens, norm_gain=norm_gain, window_query=window_query, window_key=window_key, window_value=window_value, window_gate=window_gate, window_sink=window_sink, pair_query=pair_query, pair_key=pair_key, pair_value=pair_value, pair_gate=pair_gate, map_lambda=map_lambda, head_gain=head_gain, window_out=window_out, pair_out=pair_out)


norm_eps = 1e-06
head_scale = 0.8

def row_norm(values, gain_vec):
    squares = lax.optimization_barrier(jnp.mean(values * values, axis=-1, keepdims=True))
    return values * lax.rsqrt(squares + norm_eps) * gain_vec

def reference(tokens, norm_gain, window_query, window_key, window_value, window_gate, window_sink, pair_query, pair_key, pair_value, pair_gate, map_lambda, head_gain, window_out, pair_out):
    seq_len = tokens.shape[0]
    normed = row_norm(tokens.astype(jnp.float32), norm_gain).astype(jnp.bfloat16)

    def project(weight):
        return jnp.dot(normed.astype(jnp.float32), weight.astype(jnp.float32), preferred_element_type=jnp.float32).astype(jnp.bfloat16)
    slide_query = project(window_query)
    slide_key = project(window_key)
    slide_value = project(window_value)
    slide_gate = project(window_gate)
    paired_query = project(pair_query)
    paired_key = project(pair_key)
    paired_value = project(pair_value)
    paired_gate = project(pair_gate)
    scale = HD ** (-0.5)
    group_size = A_HEADS // A_KV
    blocks_count = seq_len // WINDOW
    queries = slide_query.reshape(blocks_count, WINDOW, A_KV, group_size, HD).astype(jnp.float32)

    def band(values):
        before = jnp.pad(values, ((WINDOW, 0), (0, 0)))[:seq_len]
        return jnp.concatenate([before.reshape(blocks_count, WINDOW, A_KV, HD), values.reshape(blocks_count, WINDOW, A_KV, HD)], axis=1).astype(jnp.float32)
    band_keys = band(slide_key)
    band_values = band(slide_value)
    sink_logit = window_sink.reshape(A_KV, group_size)[:, :, None, None]
    query_idx = jnp.arange(WINDOW, dtype=jnp.int32)[:, None]
    key_idx = jnp.arange(2 * WINDOW, dtype=jnp.int32)[None, :]
    distance = query_idx - key_idx + WINDOW

    def window_block(inputs):
        block_query, block_keys, block_values, block_number = inputs
        scores = jnp.einsum('ikgd,jkd->kgij', block_query, block_keys) * scale
        valid = (distance >= 0) & (distance < WINDOW) & (block_number * WINDOW - WINDOW + key_idx >= 0)
        masked = jnp.where(valid, scores, -jnp.inf)
        top = jnp.maximum(lax.optimization_barrier(jnp.max(masked, axis=-1, keepdims=True)), sink_logit)
        weights = jnp.where(valid, jnp.exp(masked - top), 0.0)
        probs = weights / (lax.optimization_barrier(jnp.sum(weights, axis=-1, keepdims=True)) + jnp.exp(sink_logit - top))
        probs = lax.optimization_barrier(probs.astype(jnp.bfloat16)).astype(jnp.float32)
        return jnp.einsum('kgij,jkd->ikgd', probs, block_values)
    slide_out = lax.map(window_block, (queries, band_keys, band_values, jnp.arange(blocks_count, dtype=jnp.int32)))
    slide_out = slide_out.reshape(seq_len, A_HEADS * HD)
    slide_mix = (slide_out * jax.nn.silu(slide_gate.astype(jnp.float32))).astype(jnp.bfloat16)
    q_block = math.gcd(seq_len, 256)
    pair_queries = paired_query.reshape(seq_len, B_HEADS, 2, HD).astype(jnp.float32)
    pair_keys = paired_key.reshape(seq_len, B_HEADS, 2, HD).astype(jnp.float32)
    pair_values = paired_value.reshape(seq_len, B_HEADS, 2 * HD).astype(jnp.float32)
    key_pos = jnp.arange(seq_len, dtype=jnp.int32)

    def pair_block(block_number):
        begin = block_number * q_block
        block_query = lax.dynamic_slice_in_dim(pair_queries, begin, q_block, 0)
        query_pos = begin + jnp.arange(q_block, dtype=jnp.int32)
        scores = jnp.einsum('ihcd,jhcd->hcij', block_query, pair_keys) * scale
        causal = query_pos[:, None] >= key_pos[None, :]
        masked = jnp.where(causal, scores, -jnp.inf)
        top = lax.optimization_barrier(jnp.max(masked, axis=-1, keepdims=True))
        weights = jnp.where(causal, jnp.exp(masked - top), 0.0)
        totals = lax.optimization_barrier(jnp.sum(weights, axis=-1))
        rounded = lax.optimization_barrier(weights.astype(jnp.bfloat16)).astype(jnp.float32)
        numer = jnp.einsum('hcij,jhe->hcie', rounded, pair_values)
        return numer / totals[..., None]
    per_map = lax.map(pair_block, jnp.arange(seq_len // q_block, dtype=jnp.int32))
    differ = per_map[:, :, 0] - map_lambda[None, :, None, None] * per_map[:, :, 1]
    head_out = row_norm(differ, head_gain) * head_scale
    head_out = jnp.transpose(head_out, (0, 2, 1, 3)).reshape(seq_len, B_HEADS, 2 * HD)
    gate_act = jax.nn.silu(paired_gate.astype(jnp.float32).reshape(seq_len, B_HEADS, 2 * HD))
    paired_mix = (head_out * gate_act).reshape(seq_len, B_HEADS * 2 * HD).astype(jnp.bfloat16)
    slide_cols = A_HEADS * HD // HEAD_GROUPS
    paired_cols = B_HEADS * 2 * HD // HEAD_GROUPS
    total = jnp.zeros((seq_len, D), jnp.float32)
    for group_index in range(HEAD_GROUPS):
        slide_part = slide_mix[:, group_index * slide_cols:(group_index + 1) * slide_cols]
        paired_part = paired_mix[:, group_index * paired_cols:(group_index + 1) * paired_cols]
        partial_sum = jnp.dot(slide_part.astype(jnp.float32), window_out[group_index * slide_cols:(group_index + 1) * slide_cols].astype(jnp.float32), preferred_element_type=jnp.float32)
        partial_sum = partial_sum + jnp.dot(paired_part.astype(jnp.float32), pair_out[group_index * paired_cols:(group_index + 1) * paired_cols].astype(jnp.float32), preferred_element_type=jnp.float32)
        total = total + lax.optimization_barrier(partial_sum.astype(jnp.bfloat16)).astype(jnp.float32)
    return total.astype(jnp.bfloat16)
```

```python
import functools

import jax
import jax.numpy as jnp
from jax import lax
from jax.experimental import pallas as pl
from jax.experimental.pallas import tpu as pltpu
from jax.sharding import PartitionSpec as P

HD = 64
WINDOW = 128

norm_eps = 1e-06
head_scale = 0.8
CHUNK = 8
ONES = 16

MESH = pl.DeviceIdType.MESH
F32 = jnp.float32
BF16 = jnp.bfloat16


def dot_nt(a, b):
    return lax.dot_general(a, b, (((1,), (1,)), ((), ())), preferred_element_type=F32)


def dot_tn(a, b):
    return lax.dot_general(a, b, (((0,), (0,)), ((), ())), preferred_element_type=F32)


def silu(v):
    return v / (1.0 + jnp.exp(-v))


def kernel(
    S,
    T,
    tokens,
    gain_h,
    wq_h,
    wk_h,
    wv_h,
    wg_h,
    sink,
    pq_h,
    pk_h,
    pv_h,
    pg_h,
    lam_h,
    head_gain_h,
    wo_h,
    po_h,
    out_own,
    out_in,
    wq,
    wk,
    wv,
    wg,
    pq,
    pk,
    pv,
    pg,
    wo,
    po,
    norm_gain,
    head_gain,
    lam_all,
    tok_buf,
    normed,
    band_k,
    band_v,
    sq_buf,
    sg_buf,
    pg_buf,
    slide_mix,
    paired_mix,
    k_send,
    v_send,
    q_send,
    k_all,
    v_all,
    q_all,
    s_buf,
    p_buf,
    own_acc,
    own_top,
    up_acc,
    up_top,
    stat_send,
    stat_in,
    share_send,
    share_in,
    coef_send,
    coef_in,
    ret_send,
    ret_all,
    part,
    part_bf,
    w_sem,
    in_sem,
    tok_s,
    tok_r,
    lam_s,
    lam_r,
    kv_s,
    fw_s,
    kv_r,
    q_s,
    q_r,
    tail_s,
    tail_r,
    stat_s,
    stat_r,
    share_s,
    share_r,
    coef_s,
    coef_r,
    ret_s,
    ret_r,
    rs_s,
    rs_r,
):
    R, Dl = tokens.shape
    D = Dl * T
    H = k_send.shape[0]
    C = 2 * HD
    E = S // 2
    PC = E // (H * T)
    NQ = PC * T
    KB = E // NQ
    s = lax.axis_index("sp")
    t = lax.axis_index("tp")
    half = s // E
    e = lax.rem(s, E)
    ph = lax.rem(e, PC)
    th = lax.rem(e // PC, T)
    jh = e // NQ
    share = ph * T + t

    def block(k):
        return k * NQ + (share if k % 2 == 0 else NQ - 1 - share)

    my_k = e // NQ
    my_r = lax.rem(e, NQ)
    my_share = jnp.where(lax.rem(my_k, 2) == 0, my_r, NQ - 1 - my_r)
    my_p = my_share // T
    my_c = lax.rem(my_share, T)
    my_rc = lax.rem(e, T)

    def dev(sp, tp):
        return {"sp": sp, "tp": tp}

    def remote(src, dst, ss, rs, device):
        return pltpu.make_async_remote_copy(src, dst, ss, rs, device_id=device, device_id_type=MESH)

    class Send:
        def __init__(self, here, src, dst, ss, rs, device):
            self.here = here
            self.near = lambda: pltpu.make_async_copy(src, dst, rs)
            self.far = lambda: remote(src, dst, ss, rs, device)

        def start(self):
            @pl.when(self.here)
            def _():
                self.near().start()

            @pl.when(jnp.logical_not(self.here))
            def _():
                self.far().start()

        def wait_send(self):
            @pl.when(jnp.logical_not(self.here))
            def _():
                self.far().wait_send()

    def arrived(ref, ss, rs):
        remote(ref, ref, ss, rs, dev(lax.rem(s + 1, S), t)).wait_recv()

    barrier = pltpu.get_barrier_semaphore()

    def greet(d, _):
        f = lax.rem(s * T + t + d, S * T)
        pl.semaphore_signal(barrier, inc=1, device_id=dev(f // T, lax.rem(f, T)), device_id_type=MESH)
        return 0

    own_tok = pltpu.make_async_copy(tokens, tok_buf.at[t], in_sem.at[0])
    own_tok.start()
    lax.fori_loop(1, S * T, greet, 0)
    small = [
        pltpu.make_async_copy(gain_h, norm_gain, in_sem.at[1]),
        pltpu.make_async_copy(head_gain_h, head_gain, in_sem.at[2]),
        pltpu.make_async_copy(lam_h, lam_all.at[t], in_sem.at[3]),
    ]
    for cp in small:
        cp.start()
    pairs = [(pk_h, pk), (pq_h, pq), (pv_h, pv), (wk_h, wk), (wv_h, wv), (wq_h, wq), (wg_h, wg), (pg_h, pg), (wo_h, wo), (po_h, po)]
    loads = [pltpu.make_async_copy(a, b, w_sem.at[i]) for i, (a, b) in enumerate(pairs)]
    with jax.named_scope("own_tok"):
        own_tok.wait()
        for cp in small:
            cp.wait()
    for cp in loads:
        cp.start()
    with jax.named_scope("barrier"):
        pl.semaphore_wait(barrier, S * T - 1)

    Rn = R // 2

    def tok_copy(dt, h):
        at = tok_buf.at[t, pl.ds(h * Rn, Rn)]
        return remote(at, at, tok_s.at[dt, h], tok_r.at[dt, h], dev(s, lax.rem(t + dt, T)))

    def tok_in(dt, h):
        at = tok_buf.at[lax.rem(t + T - dt, T), pl.ds(h * Rn, Rn)]
        return remote(at, at, tok_s.at[dt, h], tok_r.at[dt, h], dev(s, lax.rem(t + dt, T)))

    def lam_copy(dt):
        at = lam_all.at[t]
        return remote(at, at, lam_s.at[dt], lam_r.at[dt], dev(s, lax.rem(t + dt, T)))

    def lam_in(dt):
        at = lam_all.at[lax.rem(t + T - dt, T)]
        return remote(at, at, lam_s.at[dt], lam_r.at[dt], dev(s, lax.rem(t + dt, T)))

    for h in range(2):
        for dt in range(1, T):
            tok_copy(dt, h).start()
    for dt in range(1, T):
        lam_copy(dt).start()

    NB = 32

    def norm_rows(i, _):
        rows = pl.ds(pl.multiple_of(i * NB, NB), NB)
        xs = [tok_buf[k, rows, :].astype(F32) for k in range(T)]
        total = sum(jnp.sum(x * x, axis=-1, keepdims=True) for x in xs)
        r = lax.rsqrt(total * (1.0 / D) + norm_eps)
        for k in range(T):
            cols = slice(k * Dl, (k + 1) * Dl)
            normed[rows, cols] = (xs[k] * r * norm_gain[:, cols]).astype(BF16)
        return 0

    for h in range(2):
        with jax.named_scope(f"tok{h}"):
            for dt in range(1, T):
                tok_in(dt, h).wait_recv()
        with jax.named_scope(f"norm{h}"):
            lax.fori_loop(h * Rn // NB, (h + 1) * Rn // NB, norm_rows, 0)

    def project(i, store):
        loads[i].wait()
        w = pairs[i][1]
        cols = w.shape[1]
        tile = min(256, cols)
        for c in range(0, cols, tile):
            r = jnp.dot(normed[...], w[:, c : c + tile], preferred_element_type=F32).astype(BF16)
            store(c, tile, r)

    def by_head(put):
        def store(c, tile, r):
            for o in range(0, tile, C):
                put((c + o) // C, r[:, o : o + C])

        return store

    scale = HD**-0.5

    def put_k(j, r):
        k_send[j] = r

    def put_v(j, r):
        v_send[j] = r.T

    def put_q(j, r):
        q_send[j] = (r * scale).T

    def kv_copies(i):
        src, dst = (k_send, k_all) if i == 0 else (v_send, v_all)
        out = []
        for j in range(H):
            for p in range(PC):
                to = (j * T + t) * PC + p
                here = (to == e) & (my_rc == t)
                out.append(
                    Send(here, src.at[j], dst.at[e], kv_s.at[i, j * PC + p], kv_r.at[i, e], dev(half * E + to, my_rc))
                )
        return out

    def q_copies(i):
        out = []
        for j in range(H):
            to = (j * T + t) * PC + my_p
            here = (i == 0) & (to == e) & (my_c == t)
            base = half * E if i == 0 else 0
            out.append(
                Send(here, q_send.at[j], q_all.at[i, my_k], q_s.at[i, j], q_r.at[i, my_k], dev(base + to, my_c))
            )
        return out

    def slot(i, n):
        return (k_all if i == 0 else v_all).at[n], kv_r.at[i, n]

    def relay_block(n):
        return lax.rem(e // T + n, E // T) * T + t

    def relay_copy(i, n, dt):
        b = relay_block(n)
        ref, rs = slot(i, b)
        return remote(ref, ref, fw_s.at[i, n, dt], rs, dev(s, lax.rem(t + dt, T)))

    def relay(i, first, last):
        def one(n, _):
            ref, rs = slot(i, relay_block(n))
            arrived(ref, fw_s.at[i, n, 0], rs)
            for dt in range(1, T):
                relay_copy(i, n, dt).start()
            return 0

        with jax.named_scope(f"relay{i}"):
            lax.fori_loop(first, last, one, 0)

    with jax.named_scope("proj_k"):
        project(0, by_head(put_k))
        for cp in kv_copies(0):
            cp.start()
    with jax.named_scope("proj_q"):
        project(1, by_head(put_q))

        @pl.when(half == 1)
        def _():
            for cp in q_copies(1):
                cp.start()

        for cp in q_copies(0):
            cp.start()

    with jax.named_scope("proj_v"):
        project(2, by_head(put_v))
        for cp in kv_copies(1):
            cp.start()

    def into(ref, first=0):
        def store(c, tile, r):
            ref[first:, c : c + tile] = r

        return store

    with jax.named_scope("proj_band"):
        project(3, into(band_k, WINDOW))
        project(4, into(band_v, WINDOW))

    def tails():
        return [
            remote(
                b.at[pl.ds(R, WINDOW)], b.at[pl.ds(0, WINDOW)], tail_s.at[i], tail_r.at[i], dev(lax.rem(s + 1, S), t)
            )
            for i, b in enumerate((band_k, band_v))
        ]

    @pl.when(s < S - 1)
    def _():
        for cp in tails():
            cp.start()

    @pl.when(s == 0)
    def _():
        band_k[0:WINDOW] = jnp.zeros((WINDOW, band_k.shape[1]), BF16)
        band_v[0:WINDOW] = jnp.zeros((WINDOW, band_v.shape[1]), BF16)

    n_relay = E // T
    relay(0, 0, n_relay // 2)
    with jax.named_scope("proj_sq"):
        project(5, into(sq_buf))
    relay(0, n_relay // 2, n_relay)

    def peers(i):
        def one(n, _):
            b = lax.rem(e // T + n // (T - 1), E // T) * T + lax.rem(t + 1 + lax.rem(n, T - 1), T)
            ref, rs = slot(i, b)
            arrived(ref, fw_s.at[i, 0, 0], rs)
            return 0

        with jax.named_scope(f"peers{i}"):
            lax.fori_loop(0, n_relay * (T - 1), one, 0)

    peers(0)
    with jax.named_scope("q_wait"):
        for k in range(KB):
            arrived(q_all.at[0, k], q_s.at[0, 0], q_r.at[0, k])

    row = lax.broadcasted_iota(jnp.int32, (C, R), 0)
    ones = jnp.ones((ONES, R), BF16)

    def scores(q, bs, first_masked, mine):
        zero = jnp.zeros_like(q)
        q2 = jnp.concatenate([jnp.where(row < HD, q, zero), jnp.where(row < HD, zero, q)], axis=1)
        top8 = None
        for i, b in enumerate(bs):
            st = jnp.dot(k_all[b], q2, preferred_element_type=F32)
            if b >= first_masked:
                ki = lax.broadcasted_iota(jnp.int32, (R, 2 * R), 0)
                qi = lax.rem(lax.broadcasted_iota(jnp.int32, (R, 2 * R), 1), R)
                st = jnp.where(qi - ki >= (b - mine) * R, st, -jnp.inf)
            s_buf[i] = st
            m8 = jnp.max(st.reshape(R // 8, 8, 2 * R), axis=0)
            top8 = m8 if top8 is None else jnp.maximum(top8, m8)
        return jnp.max(top8, axis=0, keepdims=True)

    def chunks_of(n):
        return [range(f, min(n, f + CHUNK)) for f in range(0, n, CHUNK)]

    def stats(k):
        total = top = None
        for bs in chunks_of(NQ * (k + 1)):
            old = top
            top = scores(q_all[0, k], bs, NQ * k, block(k))
            if old is not None:
                top = jnp.maximum(top, old)
                total = total * jnp.exp(old - top)
            for i in range(len(bs)):
                p = jnp.sum(jnp.exp(s_buf[i] - top).reshape(R // 8, 8, 2 * R), axis=0)
                total = p if total is None else total + p
        stat_send[k, 0:1] = top
        stat_send[k, 1:2] = jnp.sum(total, axis=0, keepdims=True)

    other = dev((1 - half) * E + e, t)

    def stat_copy():
        return remote(stat_send, stat_in, stat_s, stat_r, other)

    low = half == 0

    @pl.when(jnp.logical_not(low))
    def _():
        with jax.named_scope("stats"):
            for k in range(KB):
                stats(k)
            stat_copy().start()

    with jax.named_scope("proj_sg"):
        project(6, into(sg_buf))
    with jax.named_scope("proj_pg"):
        project(7, into(pg_buf))
    relay(1, 0, n_relay // 2)

    with jax.named_scope("tail"):

        @pl.when(s > 0)
        def _():
            for cp in tails():
                cp.wait_recv()

    kv_heads = band_k.shape[1] // HD
    group = sq_buf.shape[1] // band_k.shape[1]
    W = WINDOW
    blocks = R // W
    key_i = lax.broadcasted_iota(jnp.int32, (2 * W, group * W), 0)
    qry_i = lax.rem(lax.broadcasted_iota(jnp.int32, (2 * W, group * W), 1), W)
    lane_head = lax.broadcasted_iota(jnp.int32, (1, group * W), 1) // W
    dist = qry_i - key_i + W
    in_band = (dist >= 0) & (dist < W)

    def window_block(b):
        r0 = b * W
        ok = in_band & (s * R + r0 - W + key_i >= 0)
        for h in range(kv_heads):
            k = band_k[r0 : r0 + 2 * W, h * HD : (h + 1) * HD]
            v = band_v[r0 : r0 + 2 * W, h * HD : (h + 1) * HD]
            q = jnp.concatenate(
                [sq_buf[r0 : r0 + W, (h * group + g) * HD : (h * group + g + 1) * HD] for g in range(group)], axis=0
            )
            sc = jnp.where(ok, dot_nt(k, q) * scale, -jnp.inf)
            sk = jnp.full((1, group * W), sink[0, h * group], F32)
            for g in range(1, group):
                sk = jnp.where(lane_head == g, sink[0, h * group + g], sk)
            top = jnp.maximum(jnp.max(sc, axis=0, keepdims=True), sk)
            w = jnp.exp(sc - top)
            den = jnp.sum(w, axis=0, keepdims=True) + jnp.exp(sk - top)
            probs = (w * (1.0 / den)).astype(BF16)
            o = dot_tn(v, probs)
            o = jnp.concatenate([o[:, g * W : (g + 1) * W] for g in range(group)], axis=0).T
            cols = slice(h * group * HD, (h + 1) * group * HD)
            gate = sg_buf[r0 : r0 + W, cols].astype(F32)
            slide_mix[r0 : r0 + W, cols] = (o * silu(gate)).astype(BF16)

    for b in range(blocks):
        with jax.named_scope(f"win{b}"):
            window_block(b)
        if b == 0:
            relay(1, n_relay // 2, n_relay)

    NT = min(512, D)
    with jax.named_scope("wo"):
        loads[8].wait()
        for c in range(0, D, NT):
            part[:, c : c + NT] = jnp.dot(slide_mix[...], wo[:, c : c + NT], preferred_element_type=F32)

    for dt in range(1, T):
        lam_in(dt).wait_recv()
    lam_lane = lax.broadcasted_iota(jnp.int32, (1, H), 1)
    lam = jnp.sum(jnp.where(lam_lane == jh, lam_all[th], 0.0), axis=1, keepdims=True)

    peers(1)

    def attend(q, n, first_masked, mine, acc_ref, top_ref):
        for bs in chunks_of(n):
            top = scores(q, bs, first_masked, mine)
            if bs[0]:
                old = top_ref[...]
                top = jnp.maximum(top, old)
            for i in range(len(bs)):
                p_buf[i] = jnp.exp(s_buf[i] - top).astype(BF16)
            v = jnp.concatenate([v_all[b] for b in bs], axis=1)
            v = jnp.concatenate([v, jnp.concatenate([ones] * len(bs), axis=1)], axis=0)
            acc = jnp.dot(v, p_buf[0 : len(bs)].reshape(len(bs) * R, 2 * R), preferred_element_type=F32)
            if bs[0]:
                acc = acc + acc_ref[...] * jnp.exp(old - top)
            acc_ref[...] = acc
            top_ref[...] = top

    def own_block(k):
        with jax.named_scope(f"own{k}"):
            attend(q_all[0, k], NQ * (k + 1), NQ * k, block(k), own_acc.at[k], own_top.at[k])

    def up_block(k, _):
        with jax.named_scope("up"):
            arrived(q_all.at[1, k], q_s.at[1, 0], q_r.at[1, k])
            attend(q_all[1, k], E, E, 0, up_acc.at[k], up_top.at[k])
        return 0

    def share_copy(k):
        return remote(share_send.at[k], share_in.at[k], share_s.at[k], share_r.at[k], other)

    def coef_copy(k):
        return remote(coef_send.at[k], coef_in.at[k], coef_s.at[k], coef_r.at[k], other)

    def share_block(k, _):
        with jax.named_scope("share"):
            top = up_top[k]
            far_top = stat_in[k, 0:1]
            both = jnp.maximum(top, far_top)
            f = jnp.exp(top - both)
            far_f = jnp.exp(far_top - both)
            inv = 1.0 / (up_acc[k, C : C + 1] * f + stat_in[k, 1:2] * far_f)
            coef_send[k] = jnp.broadcast_to(far_f * inv, (8, 2 * R))
            a = up_acc[k, 0:C] * (f * inv)
            share_send[k] = (a[:, 0:R] - lam * a[:, R:]).astype(BF16)
            coef_copy(k).start()
            share_copy(k).start()
        return 0

    def ret_copy(k):
        b = block(k)
        here = (b == e) & (th == t)
        return Send(here, ret_send.at[k], ret_all.at[jh], ret_s.at[k], ret_r.at[jh], dev(half * E + b, th))

    def give_back(k, d):
        sq = jnp.mean(d * d, axis=0, keepdims=True)
        y = (d * (lax.rsqrt(sq + norm_eps) * head_scale)).T * head_gain[...]
        ret_send[k] = y.astype(BF16)
        ret_copy(k).start()

    def finish_low(k):
        with jax.named_scope(f"fin{k}"):
            a = own_acc[k, 0:C] * (1.0 / own_acc[k, C : C + 1])
            give_back(k, a[:, 0:R] - lam * a[:, R:])

    def finish_high(k):
        with jax.named_scope(f"share_wait{k}"):
            arrived(coef_in.at[k], coef_s.at[k], coef_r.at[k])
            arrived(share_in.at[k], share_s.at[k], share_r.at[k])
        a = own_acc[k, 0:C] * coef_in[k, 0:1]
        give_back(k, a[:, 0:R] - lam * a[:, R:] + share_in[k].astype(F32))

    @pl.when(low)
    def _():
        up_block(0, 0)
        with jax.named_scope("stat_wait"):
            arrived(stat_in, stat_s, stat_r)
        share_block(0, 0)

        def both(k, _):
            up_block(k, 0)
            share_block(k, 0)
            return 0

        lax.fori_loop(1, KB, both, 0)

    for k in range(KB):
        own_block(k)

        @pl.when(low)
        def _(k=k):
            finish_low(k)

    @pl.when(jnp.logical_not(low))
    def _():
        for k in range(KB):
            finish_high(k)

    with jax.named_scope("ret_wait"):
        for j in range(H):
            arrived(ret_all.at[j], ret_s.at[0], ret_r.at[j])
    for j in range(H):
        cols = slice(j * C, (j + 1) * C)
        gate = pg_buf[:, cols].astype(F32)
        paired_mix[:, cols] = (ret_all[j].astype(F32) * silu(gate)).astype(BF16)
    loads[9].wait()
    Rt = R // T
    chunks = range(0, D, NT)

    def rs_copy(dt, i):
        cols = pl.ds(i * NT, NT)
        return remote(
            part_bf.at[lax.rem(t + dt, T), :, cols],
            out_in.at[dt - 1, :, cols],
            rs_s.at[dt, i],
            rs_r.at[dt, i],
            dev(s, lax.rem(t + dt, T)),
        )

    def own_out(i):
        cols = pl.ds(i * NT, NT)
        return pltpu.make_async_copy(part_bf.at[t, :, cols], out_own.at[:, cols], rs_s.at[0, i])

    with jax.named_scope("po"):
        for i, c in enumerate(chunks):
            r = part[:, c : c + NT] + jnp.dot(paired_mix[...], po[:, c : c + NT], preferred_element_type=F32)
            r = r.astype(BF16)
            for k in range(T):
                part_bf[k, :, c : c + NT] = r[k * Rt : (k + 1) * Rt]
            for dt in range(1, T):
                rs_copy(dt, i).start()
            own_out(i).start()

    with jax.named_scope("drain"):
        for h in range(2):
            for dt in range(1, T):
                tok_copy(dt, h).wait_send()
        for dt in range(1, T):
            lam_copy(dt).wait_send()
        for i in range(2):
            for cp in kv_copies(i):
                cp.wait_send()

            def fw_drain(n, _, i=i):
                for dt in range(1, T):
                    relay_copy(i, n, dt).wait_send()
                return 0

            lax.fori_loop(0, n_relay, fw_drain, 0)
        for cp in q_copies(0):
            cp.wait_send()

        @pl.when(half == 1)
        def _():
            for cp in q_copies(1):
                cp.wait_send()
            stat_copy().wait_send()

        @pl.when(low)
        def _():
            for k in range(KB):
                coef_copy(k).wait_send()
                share_copy(k).wait_send()

        for k in range(KB):
            ret_copy(k).wait_send()

        @pl.when(s < S - 1)
        def _():
            for cp in tails():
                cp.wait_send()

    with jax.named_scope("rs_wait"):
        for i in range(D // NT):
            own_out(i).wait()
            for dt in range(1, T):
                rs_copy(dt, i).wait_send()
                rs_copy(dt, i).wait_recv()


def per_device(S, T, tokens, norm_gain, wq, wk, wv, wg, sink, pq, pk, pv, pg, lam, head_gain, wo, po):
    R, Dl = tokens.shape
    D = Dl * T
    A = wq.shape[1]
    KC = wk.shape[1]
    B = pq.shape[1]
    C = 2 * HD
    H = B // C
    E = S // 2
    PC = E // (H * T)
    KB = E // (PC * T)
    if S % 2 or PC * H * T != E:
        raise ValueError("unsupported mesh")
    Rt = R // T
    NC = D // min(512, D)
    smem = pl.BlockSpec(memory_space=pltpu.SMEM)
    hbm = pl.BlockSpec(memory_space=pl.ANY)
    dma = pltpu.SemaphoreType.DMA
    V = pltpu.VMEM
    scratch = [V(w.shape, BF16) for w in (wq, wk, wv, wg, pq, pk, pv, pg, wo, po)]
    scratch += [
        V((1, D), F32),
        V((1, C), F32),
        V((T, 1, H), F32),
        V((T, R, Dl), BF16),
        V((R, D), BF16),
        V((WINDOW + R, KC), BF16),
        V((WINDOW + R, KC), BF16),
        V((R, A), BF16),
        V((R, A), BF16),
        V((R, B), BF16),
        V((R, A), BF16),
        V((R, B), BF16),
        V((H, R, C), BF16),
        V((H, C, R), BF16),
        V((H, C, R), BF16),
        V((E, R, C), BF16),
        V((E, C, R), BF16),
        V((2, KB, C, R), BF16),
        V((min(E, CHUNK), R, 2 * R), F32),
        V((min(E, CHUNK), R, 2 * R), BF16),
        V((KB, C + ONES, 2 * R), F32),
        V((KB, 1, 2 * R), F32),
        V((KB, C + ONES, 2 * R), F32),
        V((KB, 1, 2 * R), F32),
        V((KB, 8, 2 * R), F32),
        V((KB, 8, 2 * R), F32),
        V((KB, C, R), BF16),
        V((KB, C, R), BF16),
        V((KB, 8, 2 * R), F32),
        V((KB, 8, 2 * R), F32),
        V((KB, R, C), BF16),
        V((H, R, C), BF16),
        V((R, D), F32),
        V((T, Rt, D), BF16),
        dma((10,)),
        dma((4,)),
        dma((T, 2)),
        dma((T, 2)),
        dma((T,)),
        dma((T,)),
        dma((2, H * PC)),
        dma((2, E // T, T)),
        dma((2, E)),
        dma((2, H)),
        dma((2, KB)),
        dma((2,)),
        dma((2,)),
        dma,
        dma,
        dma((KB,)),
        dma((KB,)),
        dma((KB,)),
        dma((KB,)),
        dma((KB,)),
        dma((H,)),
        dma((T, NC)),
        dma((T, NC)),
    ]
    own, others = pl.pallas_call(
        functools.partial(kernel, S, T),
        out_shape=[jax.ShapeDtypeStruct((Rt, D), BF16), jax.ShapeDtypeStruct((T - 1, Rt, D), BF16)],
        in_specs=[hbm, hbm, hbm, hbm, hbm, hbm, smem, hbm, hbm, hbm, hbm, hbm, hbm, hbm, hbm],
        out_specs=[hbm, hbm],
        scratch_shapes=scratch,
        compiler_params=pltpu.CompilerParams(
            collective_id=0, has_side_effects=True, vmem_limit_bytes=60 * 1024 * 1024
        ),
        name="layer",
    )(
        tokens,
        norm_gain.reshape(1, D),
        wq,
        wk,
        wv,
        wg,
        sink.reshape(1, -1),
        pq,
        pk,
        pv,
        pg,
        lam.reshape(1, -1),
        head_gain.reshape(1, -1),
        wo,
        po,
    )
    return (own.astype(F32) + jnp.sum(others.astype(F32), axis=0)).astype(BF16)


def solution(mesh):
    S, T = mesh.shape["sp"], mesh.shape["tp"]
    in_specs = (
        P("sp", "tp"),
        P(),
        P(None, "tp"),
        P(None, "tp"),
        P(None, "tp"),
        P(None, "tp"),
        P("tp"),
        P(None, "tp"),
        P(None, "tp"),
        P(None, "tp"),
        P(None, "tp"),
        P("tp"),
        P(),
        P("tp", None),
        P("tp", None),
    )
    return jax.shard_map(
        functools.partial(per_device, S, T),
        mesh=mesh,
        in_specs=in_specs,
        out_specs=P(("sp", "tp"), None),
        check_vma=False,
    )
```

```python
import functools

import jax
import jax.numpy as jnp
from jax import lax
from jax.experimental import pallas as pl
from jax.experimental.pallas import tpu as pltpu
from jax.sharding import PartitionSpec as P

HD = 64
WINDOW = 128

norm_eps = 1e-06
head_scale = 0.8
CHUNK = 8
ONES = 16

MESH = pl.DeviceIdType.MESH
F32 = jnp.float32
BF16 = jnp.bfloat16


def dot_nt(a, b):
    return lax.dot_general(a, b, (((1,), (1,)), ((), ())), preferred_element_type=F32)


def dot_tn(a, b):
    return lax.dot_general(a, b, (((0,), (0,)), ((), ())), preferred_element_type=F32)


def silu(v):
    return v / (1.0 + jnp.exp(-v))


def kernel(
    S,
    T,
    tokens,
    gain_h,
    wq_h,
    wk_h,
    wv_h,
    wg_h,
    sink,
    pq_h,
    pk_h,
    pv_h,
    pg_h,
    lam_h,
    head_gain_h,
    wo_h,
    po_h,
    out_own,
    out_in,
    wq,
    wk,
    wv,
    wg,
    pq,
    pk,
    pv,
    pg,
    wo,
    po,
    norm_gain,
    head_gain,
    lam_all,
    tok_buf,
    normed,
    band_k,
    band_v,
    sq_buf,
    sg_buf,
    pg_buf,
    slide_mix,
    paired_mix,
    k_send,
    v_send,
    q_send,
    k_all,
    v_all,
    q_all,
    s_buf,
    p_buf,
    own_acc,
    own_top,
    up_acc,
    up_top,
    stat_send,
    stat_in,
    share_send,
    share_in,
    coef_send,
    coef_in,
    ret_send,
    ret_all,
    part,
    part_bf,
    w_sem,
    in_sem,
    tok_s,
    tok_r,
    lam_s,
    lam_r,
    kv_s,
    fw_s,
    kv_r,
    q_s,
    q_r,
    tail_s,
    tail_r,
    stat_s,
    stat_r,
    share_s,
    share_r,
    coef_s,
    coef_r,
    ret_s,
    ret_r,
    rs_s,
    rs_r,
):
    R, Dl = tokens.shape
    D = Dl * T
    H = k_send.shape[0]
    C = 2 * HD
    E = S // 2
    PC = E // (H * T)
    NQ = PC * T
    KB = E // NQ

    def goes_up(j):
        return False

    ups = [j for j in range(H) if goes_up(j)]
    downs = [j for j in range(H) if not goes_up(j)]
    s = lax.axis_index("sp")
    t = lax.axis_index("tp")
    half = s // E
    e = lax.rem(s, E)
    ph = lax.rem(e, PC)
    th = lax.rem(e // PC, T)
    jh = e // NQ
    share = ph * T + t

    low = half == 0
    keys_up = functools.reduce(jnp.logical_or, [jh == j for j in ups], jh < 0)
    up_core = jnp.logical_not(low) & keys_up
    down_core = low & jnp.logical_not(keys_up)
    asking_core = jnp.logical_not(low) & jnp.logical_not(keys_up)

    def block(k):
        return k * NQ + jnp.where(lax.rem(k, 2) == 0, share, NQ - 1 - share)

    my_k = e // NQ
    my_r = lax.rem(e, NQ)
    my_share = jnp.where(lax.rem(my_k, 2) == 0, my_r, NQ - 1 - my_r)
    my_p = my_share // T
    my_c = lax.rem(my_share, T)
    my_rc = lax.rem(e, T)

    def dev(sp, tp):
        return {"sp": sp, "tp": tp}

    def remote(src, dst, ss, rs, device):
        return pltpu.make_async_remote_copy(src, dst, ss, rs, device_id=device, device_id_type=MESH)

    class Send:
        def __init__(self, here, src, dst, ss, rs, device):
            self.here = here
            self.near = lambda: pltpu.make_async_copy(src, dst, rs)
            self.far = lambda: remote(src, dst, ss, rs, device)

        def start(self):
            @pl.when(self.here)
            def _():
                self.near().start()

            @pl.when(jnp.logical_not(self.here))
            def _():
                self.far().start()

        def wait_send(self):
            @pl.when(jnp.logical_not(self.here))
            def _():
                self.far().wait_send()

    def arrived(ref, ss, rs):
        remote(ref, ref, ss, rs, dev(lax.rem(s + 1, S), t)).wait_recv()

    barrier = pltpu.get_barrier_semaphore()

    def greet(d, _):
        f = lax.rem(s * T + t + d, S * T)
        pl.semaphore_signal(barrier, inc=1, device_id=dev(f // T, lax.rem(f, T)), device_id_type=MESH)
        return 0

    own_tok = pltpu.make_async_copy(tokens, tok_buf.at[t], in_sem.at[0])
    own_tok.start()
    lax.fori_loop(1, S * T, greet, 0)
    small = [
        pltpu.make_async_copy(gain_h, norm_gain, in_sem.at[1]),
        pltpu.make_async_copy(head_gain_h, head_gain, in_sem.at[2]),
        pltpu.make_async_copy(lam_h, lam_all.at[t], in_sem.at[3]),
    ]
    for cp in small:
        cp.start()
    pairs = [(pk_h, pk), (pv_h, pv), (pq_h, pq), (wk_h, wk), (wv_h, wv), (wq_h, wq), (wg_h, wg), (pg_h, pg), (wo_h, wo), (po_h, po)]
    loads = [pltpu.make_async_copy(a, b, w_sem.at[i]) for i, (a, b) in enumerate(pairs)]
    with jax.named_scope("own_tok"):
        own_tok.wait()
        for cp in small:
            cp.wait()
    for cp in loads:
        cp.start()
    with jax.named_scope("barrier"):
        pl.semaphore_wait(barrier, S * T - 1)

    Rn = R // 2

    def tok_copy(dt, h):
        at = tok_buf.at[t, pl.ds(h * Rn, Rn)]
        return remote(at, at, tok_s.at[dt, h], tok_r.at[dt, h], dev(s, lax.rem(t + dt, T)))

    def tok_in(dt, h):
        at = tok_buf.at[lax.rem(t + T - dt, T), pl.ds(h * Rn, Rn)]
        return remote(at, at, tok_s.at[dt, h], tok_r.at[dt, h], dev(s, lax.rem(t + dt, T)))

    def lam_copy(dt):
        at = lam_all.at[t]
        return remote(at, at, lam_s.at[dt], lam_r.at[dt], dev(s, lax.rem(t + dt, T)))

    def lam_in(dt):
        at = lam_all.at[lax.rem(t + T - dt, T)]
        return remote(at, at, lam_s.at[dt], lam_r.at[dt], dev(s, lax.rem(t + dt, T)))

    for h in range(2):
        for dt in range(1, T):
            tok_copy(dt, h).start()
    for dt in range(1, T):
        lam_copy(dt).start()

    NB = 32

    def norm_rows(i, _):
        rows = pl.ds(pl.multiple_of(i * NB, NB), NB)
        xs = [tok_buf[k, rows, :].astype(F32) for k in range(T)]
        total = sum(jnp.sum(x * x, axis=-1, keepdims=True) for x in xs)
        r = lax.rsqrt(total * (1.0 / D) + norm_eps)
        for k in range(T):
            cols = slice(k * Dl, (k + 1) * Dl)
            normed[rows, cols] = (xs[k] * r * norm_gain[:, cols]).astype(BF16)
        return 0

    for h in range(2):
        with jax.named_scope(f"tok{h}"):
            for dt in range(1, T):
                tok_in(dt, h).wait_recv()
        with jax.named_scope(f"norm{h}"):
            lax.fori_loop(h * Rn // NB, (h + 1) * Rn // NB, norm_rows, 0)

    def project(i, store):
        loads[i].wait()
        w = pairs[i][1]
        cols = w.shape[1]
        tile = min(256, cols)
        for c in range(0, cols, tile):
            r = jnp.dot(normed[...], w[:, c : c + tile], preferred_element_type=F32).astype(BF16)
            store(c, tile, r)

    def by_head(put):
        def store(c, tile, r):
            for o in range(0, tile, C):
                put((c + o) // C, r[:, o : o + C])

        return store

    scale = HD**-0.5

    def put_k(j, r):
        k_send[j] = r

    def put_v(j, r):
        v_send[j] = r.T

    def put_q(j, r):
        q_send[j] = (r * scale).T

    def kv_copies(i, up, heads):
        src, dst = (k_send, k_all) if i == 0 else (v_send, v_all)
        out = []
        for j in heads:
            for p in range(PC):
                to = (j * T + t) * PC + p
                here = (up == 0) & (to == e) & (my_rc == t)
                base = E if up else half * E
                ss = kv_s.at[i, up, j * PC + p]
                out.append(Send(here, src.at[j], dst.at[up, e], ss, kv_r.at[i, up, e], dev(base + to, my_rc)))
        return out

    def q_copies(i, heads):
        out = []
        for j in heads:
            to = (j * T + t) * PC + my_p
            here = (i == 0) & (to == e) & (my_c == t)
            base = half * E if i == 0 else 0
            out.append(
                Send(here, q_send.at[j], q_all.at[i, my_k], q_s.at[i, j], q_r.at[i, my_k], dev(base + to, my_c))
            )
        return out

    n_relay = E // T

    def slot(i, up, n):
        return (k_all if i == 0 else v_all).at[up, n], kv_r.at[i, up, n]

    def relay_block(up, n, core):
        first = n_relay - 1 - n if up else lax.rem(e // T + n, n_relay)
        return first * T + core

    def relay_copy(i, up, n, dt):
        ref, rs = slot(i, up, relay_block(up, n, t))
        return remote(ref, ref, fw_s.at[i, up, n, dt], rs, dev(s, lax.rem(t + dt, T)))

    def relay(i, first, last, up=0):
        def one(n, _):
            ref, rs = slot(i, up, relay_block(up, n, t))
            arrived(ref, fw_s.at[i, up, n, 0], rs)
            for dt in range(1, T):
                relay_copy(i, up, n, dt).start()
            return 0

        with jax.named_scope(f"relay{i}{up}"):
            lax.fori_loop(first, last, one, 0)

    def peers(i, first, last, up=0):
        def one(n, _):
            core = lax.rem(t + 1 + lax.rem(n, T - 1), T)
            ref, rs = slot(i, up, relay_block(up, n // (T - 1), core))
            arrived(ref, fw_s.at[i, up, 0, 0], rs)
            return 0

        with jax.named_scope(f"peers{i}{up}"):
            lax.fori_loop(first * (T - 1), last * (T - 1), one, 0)

    def begin(copies):
        for cp in copies:
            cp.start()

    def begin(copies):
        for cp in copies:
            cp.start()

    high = jnp.logical_not(low)

    with jax.named_scope("proj_k"):
        project(0, by_head(put_k))

        @pl.when(high)
        def _():
            begin(kv_copies(0, 0, downs + ups))

        @pl.when(low)
        def _():
            begin(kv_copies(0, 0, downs))

    with jax.named_scope("proj_v"):
        project(1, by_head(put_v))

        @pl.when(low)
        def _():
            begin(kv_copies(1, 0, downs))
            for i in range(2):
                begin(kv_copies(i, 1, ups))

    with jax.named_scope("proj_q"):
        project(2, by_head(put_q))

        @pl.when(high)
        def _():
            begin(q_copies(0, downs + ups))
            begin(q_copies(1, downs[::-1]))
            begin(kv_copies(1, 0, ups))

    def late_sends():
        @pl.when(low)
        def _():
            for i in range(2):
                begin(kv_copies(i, 0, ups))
            begin(q_copies(0, ups + downs))

        @pl.when(high)
        def _():
            begin(kv_copies(1, 0, downs))

    def into(ref, first=0):
        def store(c, tile, r):
            ref[first:, c : c + tile] = r

        return store

    with jax.named_scope("proj_band"):
        project(3, into(band_k, WINDOW))
        project(4, into(band_v, WINDOW))

    def tails():
        return [
            remote(
                b.at[pl.ds(R, WINDOW)], b.at[pl.ds(0, WINDOW)], tail_s.at[i], tail_r.at[i], dev(lax.rem(s + 1, S), t)
            )
            for i, b in enumerate((band_k, band_v))
        ]

    @pl.when(s < S - 1)
    def _():
        for cp in tails():
            cp.start()

    @pl.when(s == 0)
    def _():
        band_k[0:WINDOW] = jnp.zeros((WINDOW, band_k.shape[1]), BF16)
        band_v[0:WINDOW] = jnp.zeros((WINDOW, band_v.shape[1]), BF16)

    with jax.named_scope("proj_sq"):
        project(5, into(sq_buf))
    with jax.named_scope("proj_sg"):
        project(6, into(sg_buf))
    with jax.named_scope("proj_pg"):
        project(7, into(pg_buf))

    kv_heads = band_k.shape[1] // HD
    group = sq_buf.shape[1] // band_k.shape[1]
    W = WINDOW
    blocks = R // W
    key_i = lax.broadcasted_iota(jnp.int32, (2 * W, group * W), 0)
    qry_i = lax.rem(lax.broadcasted_iota(jnp.int32, (2 * W, group * W), 1), W)
    lane_head = lax.broadcasted_iota(jnp.int32, (1, group * W), 1) // W
    dist = qry_i - key_i + W
    in_band = (dist >= 0) & (dist < W)

    def window_block(b):
        r0 = b * W
        ok = in_band & (s * R + r0 - W + key_i >= 0)
        for h in range(kv_heads):
            k = band_k[r0 : r0 + 2 * W, h * HD : (h + 1) * HD]
            v = band_v[r0 : r0 + 2 * W, h * HD : (h + 1) * HD]
            q = jnp.concatenate(
                [sq_buf[r0 : r0 + W, (h * group + g) * HD : (h * group + g + 1) * HD] for g in range(group)], axis=0
            )
            sc = jnp.where(ok, dot_nt(k, q) * scale, -jnp.inf)
            sk = jnp.full((1, group * W), sink[0, h * group], F32)
            for g in range(1, group):
                sk = jnp.where(lane_head == g, sink[0, h * group + g], sk)
            top = jnp.maximum(jnp.max(sc, axis=0, keepdims=True), sk)
            w = jnp.exp(sc - top)
            den = jnp.sum(w, axis=0, keepdims=True) + jnp.exp(sk - top)
            probs = (w * (1.0 / den)).astype(BF16)
            o = dot_tn(v, probs)
            o = jnp.concatenate([o[:, g * W : (g + 1) * W] for g in range(group)], axis=0).T
            cols = slice(h * group * HD, (h + 1) * group * HD)
            gate = sg_buf[r0 : r0 + W, cols].astype(F32)
            slide_mix[r0 : r0 + W, cols] = (o * silu(gate)).astype(BF16)

    def other_windows():
        for b in range(1, blocks):
            with jax.named_scope(f"win{b}"):
                window_block(b)

    pl.when(low)(other_windows)
    late_sends()
    relay(0, 0, n_relay)
    peers(0, 0, n_relay)

    def queries():
        with jax.named_scope("q_wait"):
            for k in range(KB):
                arrived(q_all.at[0, k], q_s.at[0, 0], q_r.at[0, k])

    pl.when(jnp.logical_not(low))(queries)
    row = lax.broadcasted_iota(jnp.int32, (C, R), 0)
    ones = jnp.ones((ONES, R), BF16)

    def scores(q, up, bs, first_masked, mine):
        zero = jnp.zeros_like(q)
        q2 = jnp.concatenate([jnp.where(row < HD, q, zero), jnp.where(row < HD, zero, q)], axis=1)
        top8 = None
        for i, b in enumerate(bs):
            st = jnp.dot(k_all[up, b], q2, preferred_element_type=F32)
            if b >= first_masked:
                ki = lax.broadcasted_iota(jnp.int32, (R, 2 * R), 0)
                qi = lax.rem(lax.broadcasted_iota(jnp.int32, (R, 2 * R), 1), R)
                st = jnp.where(qi - ki >= (b - mine) * R, st, -jnp.inf)
            s_buf[i] = st
            m8 = jnp.max(st.reshape(R // 8, 8, 2 * R), axis=0)
            top8 = m8 if top8 is None else jnp.maximum(top8, m8)
        return jnp.max(top8, axis=0, keepdims=True)

    def chunks_of(n):
        return [range(f, min(n, f + CHUNK)) for f in range(0, n, CHUNK)]

    def stats(k):
        total = top = None
        for bs in chunks_of(NQ * (k + 1)):
            old = top
            top = scores(q_all[0, k], 0, bs, NQ * k, block(k))
            if old is not None:
                top = jnp.maximum(top, old)
                total = total * jnp.exp(old - top)
            for i in range(len(bs)):
                p = jnp.sum(jnp.exp(s_buf[i] - top).reshape(R // 8, 8, 2 * R), axis=0)
                total = p if total is None else total + p
        stat_send[k, 0:1] = top
        stat_send[k, 1:2] = jnp.sum(total, axis=0, keepdims=True)

    other = dev((1 - half) * E + e, t)

    def stat_copy():
        return remote(stat_send, stat_in, stat_s, stat_r, other)

    @pl.when(asking_core)
    def _():
        with jax.named_scope("stats"):
            for k in range(KB):
                stats(k)
            stat_copy().start()

    pl.when(high)(other_windows)

    def values():
        relay(1, 0, n_relay)
        peers(1, 0, n_relay)

    pl.when(jnp.logical_not(up_core))(values)

    for dt in range(1, T):
        lam_in(dt).wait_recv()
    lam_lane = lax.broadcasted_iota(jnp.int32, (1, H), 1)
    lam = jnp.sum(jnp.where(lam_lane == jh, lam_all[th], 0.0), axis=1, keepdims=True)

    def attend(q, up, parts, first_masked, mine, acc_ref, top_ref, fresh):
        for bs in parts:
            top = scores(q, up, bs, first_masked, mine)
            if not fresh:
                old = top_ref[...]
                top = jnp.maximum(top, old)
            for i in range(len(bs)):
                p_buf[i] = jnp.exp(s_buf[i] - top).astype(BF16)
            v = jnp.concatenate([v_all[up, b] for b in bs], axis=1)
            v = jnp.concatenate([v, jnp.concatenate([ones] * len(bs), axis=1)], axis=0)
            acc = jnp.dot(v, p_buf[0 : len(bs)].reshape(len(bs) * R, 2 * R), preferred_element_type=F32)
            if not fresh:
                acc = acc + acc_ref[...] * jnp.exp(old - top)
            acc_ref[...] = acc
            top_ref[...] = top
            fresh = False

    def own_block(k):
        with jax.named_scope(f"own{k}"):
            attend(q_all[0, k], 0, chunks_of(NQ * (k + 1)), NQ * k, block(k), own_acc.at[k], own_top.at[k], False)

    def down_block(k, _):
        with jax.named_scope("down"):
            arrived(q_all.at[1, k], q_s.at[1, 0], q_r.at[1, k])
            attend(q_all[1, k], 0, chunks_of(E), E, 0, up_acc.at[k], up_top.at[k], True)
        return 0

    def upper(parts, fresh, last):
        def one(k, _):
            with jax.named_scope("upper"):
                attend(q_all[0, k], 1, parts, E, 0, own_acc.at[k], own_top.at[k], fresh)
                if last:
                    finish_low(k)
            return 0

        lax.fori_loop(0, KB, one, 0)

    def share_copy(k):
        return remote(share_send.at[k], share_in.at[k], share_s.at[k], share_r.at[k], other)

    def coef_copy(k):
        return remote(coef_send.at[k], coef_in.at[k], coef_s.at[k], coef_r.at[k], other)

    def share_block(k, _):
        with jax.named_scope("share"):
            top = up_top[k]
            far_top = stat_in[k, 0:1]
            both = jnp.maximum(top, far_top)
            f = jnp.exp(top - both)
            far_f = jnp.exp(far_top - both)
            inv = 1.0 / (up_acc[k, C : C + 1] * f + stat_in[k, 1:2] * far_f)
            coef_send[k] = jnp.broadcast_to(far_f * inv, (8, 2 * R))
            a = up_acc[k, 0:C] * (f * inv)
            share_send[k] = (a[:, 0:R] - lam * a[:, R:]).astype(BF16)
            coef_copy(k).start()
            share_copy(k).start()
        return 0

    def ret_copy(k):
        b = block(k)
        here = (b == e) & (th == t)
        return Send(here, ret_send.at[k], ret_all.at[jh], ret_s.at[k], ret_r.at[jh], dev(half * E + b, th))

    def give_back(k, d):
        sq = jnp.mean(d * d, axis=0, keepdims=True)
        y = (d * (lax.rsqrt(sq + norm_eps) * head_scale)).T * head_gain[...]
        ret_send[k] = y.astype(BF16)
        ret_copy(k).start()

    def finish_low(k):
        with jax.named_scope("fin"):
            a = own_acc[k, 0:C] * (1.0 / own_acc[k, C : C + 1])
            give_back(k, a[:, 0:R] - lam * a[:, R:])

    def finish_high(k):
        with jax.named_scope(f"share_wait{k}"):
            arrived(coef_in.at[k], coef_s.at[k], coef_r.at[k])
            arrived(share_in.at[k], share_s.at[k], share_r.at[k])
        a = own_acc[k, 0:C] * coef_in[k, 0:1]
        give_back(k, a[:, 0:R] - lam * a[:, R:] + share_in[k].astype(F32))

    @pl.when(down_core)
    def _():
        ready = 1
        lax.fori_loop(0, ready, down_block, 0)
        with jax.named_scope("stat_wait"):
            arrived(stat_in, stat_s, stat_r)
        lax.fori_loop(0, ready, share_block, 0)
        for k in range(ready, KB):
            down_block(k, 0)
            share_block(k, 0)

    pl.when(low)(queries)
    @pl.when(jnp.logical_not(up_core))
    def _():
        own_acc[...] = jnp.zeros(own_acc.shape, F32)
        own_top[...] = jnp.full(own_top.shape, -1e30, F32)

    NT = min(512, D)

    def first_window():
        with jax.named_scope("tail"):

            @pl.when(s > 0)
            def _():
                for cp in tails():
                    cp.wait_recv()

        with jax.named_scope("win0"):
            window_block(0)
        with jax.named_scope("wo"):
            loads[8].wait()
            for c in range(0, D, NT):
                part[:, c : c + NT] = jnp.dot(slide_mix[...], wo[:, c : c + NT], preferred_element_type=F32)

    n_near = n_relay // 2
    near, far = range((n_relay - n_near) * T, E), range(0, (n_relay - n_near) * T)
    if ups:

        @pl.when(up_core)
        def _():
            for i in range(2):
                relay(i, 0, n_near, 1)
            for i in range(2):
                peers(i, 0, n_near, 1)
            upper([near], True, False)
            first_window()
            values()

    for k in range(KB):
        if k == KB // 2 and ups:

            @pl.when(up_core)
            def _():
                for i in range(2):
                    relay(i, n_near, n_relay, 1)

        own_block(k)

        @pl.when(low)
        def _(k=k):
            finish_low(k)

    if ups:

        @pl.when(up_core)
        def _():
            for i in range(2):
                peers(i, n_near, n_relay, 1)
            upper([far], False, True)

    pl.when(jnp.logical_not(up_core))(first_window)

    @pl.when(asking_core)
    def _():
        for k in range(KB):
            finish_high(k)

    with jax.named_scope("ret_wait"):
        for j in range(H):
            arrived(ret_all.at[j], ret_s.at[0], ret_r.at[j])
    for j in range(H):
        cols = slice(j * C, (j + 1) * C)
        gate = pg_buf[:, cols].astype(F32)
        paired_mix[:, cols] = (ret_all[j].astype(F32) * silu(gate)).astype(BF16)
    loads[9].wait()
    Rt = R // T
    chunks = range(0, D, NT)

    def rs_copy(dt, i):
        cols = pl.ds(i * NT, NT)
        return remote(
            part_bf.at[lax.rem(t + dt, T), :, cols],
            out_in.at[dt - 1, :, cols],
            rs_s.at[dt, i],
            rs_r.at[dt, i],
            dev(s, lax.rem(t + dt, T)),
        )

    def own_out(i):
        cols = pl.ds(i * NT, NT)
        return pltpu.make_async_copy(part_bf.at[t, :, cols], out_own.at[:, cols], rs_s.at[0, i])

    with jax.named_scope("po"):
        for i, c in enumerate(chunks):
            r = part[:, c : c + NT] + jnp.dot(paired_mix[...], po[:, c : c + NT], preferred_element_type=F32)
            r = r.astype(BF16)
            for k in range(T):
                part_bf[k, :, c : c + NT] = r[k * Rt : (k + 1) * Rt]
            for dt in range(1, T):
                rs_copy(dt, i).start()
            own_out(i).start()

    with jax.named_scope("drain"):
        for h in range(2):
            for dt in range(1, T):
                tok_copy(dt, h).wait_send()
        for dt in range(1, T):
            lam_copy(dt).wait_send()
        def relayed(up):
            def one(n, _):
                for i in range(2):
                    for dt in range(1, T):
                        relay_copy(i, up, n, dt).wait_send()
                return 0

            lax.fori_loop(0, n_relay, one, 0)

        relayed(0)
        for i in range(2):
            for cp in kv_copies(i, 0, range(H)):
                cp.wait_send()
        for cp in q_copies(0, range(H)):
            cp.wait_send()

        @pl.when(half == 1)
        def _():
            for cp in q_copies(1, downs):
                cp.wait_send()

        @pl.when(low)
        def _():
            for i in range(2):
                for cp in kv_copies(i, 1, ups):
                    cp.wait_send()

        if ups:
            pl.when(up_core)(lambda: relayed(1))

        @pl.when(asking_core)
        def _():
            stat_copy().wait_send()

        @pl.when(down_core)
        def _():
            for k in range(KB):
                coef_copy(k).wait_send()
                share_copy(k).wait_send()

        for k in range(KB):
            ret_copy(k).wait_send()

        @pl.when(s < S - 1)
        def _():
            for cp in tails():
                cp.wait_send()

    with jax.named_scope("rs_wait"):
        for i in range(D // NT):
            own_out(i).wait()
            for dt in range(1, T):
                rs_copy(dt, i).wait_send()
                rs_copy(dt, i).wait_recv()


def per_device(S, T, tokens, norm_gain, wq, wk, wv, wg, sink, pq, pk, pv, pg, lam, head_gain, wo, po):
    R, Dl = tokens.shape
    D = Dl * T
    A = wq.shape[1]
    KC = wk.shape[1]
    B = pq.shape[1]
    C = 2 * HD
    H = B // C
    E = S // 2
    PC = E // (H * T)
    KB = E // (PC * T)
    if S % 2 or PC * H * T != E:
        raise ValueError("unsupported mesh")
    Rt = R // T
    NC = D // min(512, D)
    smem = pl.BlockSpec(memory_space=pltpu.SMEM)
    hbm = pl.BlockSpec(memory_space=pl.ANY)
    dma = pltpu.SemaphoreType.DMA
    V = pltpu.VMEM
    scratch = [V(w.shape, BF16) for w in (wq, wk, wv, wg, pq, pk, pv, pg, wo, po)]
    scratch += [
        V((1, D), F32),
        V((1, C), F32),
        V((T, 1, H), F32),
        V((T, R, Dl), BF16),
        V((R, D), BF16),
        V((WINDOW + R, KC), BF16),
        V((WINDOW + R, KC), BF16),
        V((R, A), BF16),
        V((R, A), BF16),
        V((R, B), BF16),
        V((R, A), BF16),
        V((R, B), BF16),
        V((H, R, C), BF16),
        V((H, C, R), BF16),
        V((H, C, R), BF16),
        V((2, E, R, C), BF16),
        V((2, E, C, R), BF16),
        V((2, KB, C, R), BF16),
        V((min(E, CHUNK), R, 2 * R), F32),
        V((min(E, CHUNK), R, 2 * R), BF16),
        V((KB, C + ONES, 2 * R), F32),
        V((KB, 1, 2 * R), F32),
        V((KB, C + ONES, 2 * R), F32),
        V((KB, 1, 2 * R), F32),
        V((KB, 8, 2 * R), F32),
        V((KB, 8, 2 * R), F32),
        V((KB, C, R), BF16),
        V((KB, C, R), BF16),
        V((KB, 8, 2 * R), F32),
        V((KB, 8, 2 * R), F32),
        V((KB, R, C), BF16),
        V((H, R, C), BF16),
        V((R, D), F32),
        V((T, Rt, D), BF16),
        dma((10,)),
        dma((4,)),
        dma((T, 2)),
        dma((T, 2)),
        dma((T,)),
        dma((T,)),
        dma((2, 2, H * PC)),
        dma((2, 2, E // T, T)),
        dma((2, 2, E)),
        dma((2, H)),
        dma((2, KB)),
        dma((2,)),
        dma((2,)),
        dma,
        dma,
        dma((KB,)),
        dma((KB,)),
        dma((KB,)),
        dma((KB,)),
        dma((KB,)),
        dma((H,)),
        dma((T, NC)),
        dma((T, NC)),
    ]
    own, others = pl.pallas_call(
        functools.partial(kernel, S, T),
        out_shape=[jax.ShapeDtypeStruct((Rt, D), BF16), jax.ShapeDtypeStruct((T - 1, Rt, D), BF16)],
        in_specs=[hbm, hbm, hbm, hbm, hbm, hbm, smem, hbm, hbm, hbm, hbm, hbm, hbm, hbm, hbm],
        out_specs=[hbm, hbm],
        scratch_shapes=scratch,
        compiler_params=pltpu.CompilerParams(
            collective_id=0, has_side_effects=True, vmem_limit_bytes=60 * 1024 * 1024
        ),
        name="layer",
    )(
        tokens,
        norm_gain.reshape(1, D),
        wq,
        wk,
        wv,
        wg,
        sink.reshape(1, -1),
        pq,
        pk,
        pv,
        pg,
        lam.reshape(1, -1),
        head_gain.reshape(1, -1),
        wo,
        po,
    )
    return (own.astype(F32) + jnp.sum(others.astype(F32), axis=0)).astype(BF16)


def solution(mesh):
    S, T = mesh.shape["sp"], mesh.shape["tp"]
    in_specs = (
        P("sp", "tp"),
        P(),
        P(None, "tp"),
        P(None, "tp"),
        P(None, "tp"),
        P(None, "tp"),
        P("tp"),
        P(None, "tp"),
        P(None, "tp"),
        P(None, "tp"),
        P(None, "tp"),
        P("tp"),
        P(),
        P("tp", None),
        P("tp", None),
    )
    return jax.shard_map(
        functools.partial(per_device, S, T),
        mesh=mesh,
        in_specs=in_specs,
        out_specs=P(("sp", "tp"), None),
        check_vma=False,
    )
```

```python
import functools

import jax
import jax.numpy as jnp
from jax import lax
from jax.experimental import pallas as pl
from jax.experimental.pallas import tpu as pltpu
from jax.sharding import PartitionSpec as P

HD = 64
WINDOW = 128

norm_eps = 1e-06
head_scale = 0.8
CHUNK = 8
ONES = 16

MESH = pl.DeviceIdType.MESH
F32 = jnp.float32
BF16 = jnp.bfloat16


def dot_nt(a, b):
    return lax.dot_general(a, b, (((1,), (1,)), ((), ())), preferred_element_type=F32)


def dot_tn(a, b):
    return lax.dot_general(a, b, (((0,), (0,)), ((), ())), preferred_element_type=F32)


def silu(v):
    return v / (1.0 + jnp.exp(-v))


def kernel(
    S,
    T,
    tokens,
    gain_h,
    wq_h,
    wk_h,
    wv_h,
    wg_h,
    sink,
    pq_h,
    pk_h,
    pv_h,
    pg_h,
    lam_h,
    head_gain_h,
    wo_h,
    po_h,
    out_own,
    out_in,
    wq,
    wk,
    wv,
    wg,
    pq,
    pk,
    pv,
    pg,
    wo,
    po,
    norm_gain,
    head_gain,
    lam_all,
    tok_buf,
    normed,
    band_k,
    band_v,
    sq_buf,
    sg_buf,
    pg_buf,
    gate_buf,
    slide_mix,
    paired_mix,
    k_send,
    v_send,
    q_send,
    k_all,
    v_all,
    q_all,
    s_buf,
    p_buf,
    own_acc,
    own_top,
    up_acc,
    up_top,
    stat_send,
    stat_in,
    share_send,
    share_in,
    coef_send,
    coef_in,
    ret_send,
    ret_all,
    part,
    part_bf,
    w_sem,
    in_sem,
    tok_s,
    tok_r,
    lam_s,
    lam_r,
    kv_s,
    fw_s,
    kv_r,
    q_s,
    q_r,
    tail_s,
    tail_r,
    stat_s,
    stat_r,
    share_s,
    share_r,
    coef_s,
    coef_r,
    ret_s,
    ret_r,
    rs_s,
    rs_r,
):
    R, Dl = tokens.shape
    D = Dl * T
    H = k_send.shape[0]
    C = 2 * HD
    E = S // 2
    PC = E // (H * T)
    NQ = PC * T
    KB = E // NQ

    def goes_up(j):
        return False

    ups = [j for j in range(H) if goes_up(j)]
    downs = [j for j in range(H) if not goes_up(j)]
    s = lax.axis_index("sp")
    t = lax.axis_index("tp")
    half = s // E
    e = lax.rem(s, E)
    ph = lax.rem(e, PC)
    th = lax.rem(e // PC, T)
    jh = e // NQ
    share = ph * T + t

    low = half == 0
    keys_up = functools.reduce(jnp.logical_or, [jh == j for j in ups], jh < 0)
    up_core = jnp.logical_not(low) & keys_up
    down_core = low & jnp.logical_not(keys_up)
    asking_core = jnp.logical_not(low) & jnp.logical_not(keys_up)

    def block(k):
        return k * NQ + jnp.where(lax.rem(k, 2) == 0, share, NQ - 1 - share)

    my_k = e // NQ
    my_r = lax.rem(e, NQ)
    my_share = jnp.where(lax.rem(my_k, 2) == 0, my_r, NQ - 1 - my_r)
    my_p = my_share // T
    my_c = lax.rem(my_share, T)
    my_rc = lax.rem(e, T)

    def dev(sp, tp):
        return {"sp": sp, "tp": tp}

    def remote(src, dst, ss, rs, device):
        return pltpu.make_async_remote_copy(src, dst, ss, rs, device_id=device, device_id_type=MESH)

    class Send:
        def __init__(self, here, src, dst, ss, rs, device):
            self.here = here
            self.near = lambda: pltpu.make_async_copy(src, dst, rs)
            self.far = lambda: remote(src, dst, ss, rs, device)

        def start(self):
            @pl.when(self.here)
            def _():
                self.near().start()

            @pl.when(jnp.logical_not(self.here))
            def _():
                self.far().start()

        def wait_send(self):
            @pl.when(jnp.logical_not(self.here))
            def _():
                self.far().wait_send()

    def arrived(ref, ss, rs):
        remote(ref, ref, ss, rs, dev(lax.rem(s + 1, S), t)).wait_recv()

    barrier = pltpu.get_barrier_semaphore()

    def greet(d, _):
        f = lax.rem(s * T + t + d, S * T)
        pl.semaphore_signal(barrier, inc=1, device_id=dev(f // T, lax.rem(f, T)), device_id_type=MESH)
        return 0

    own_tok = pltpu.make_async_copy(tokens, tok_buf.at[t], in_sem.at[0])
    own_tok.start()
    lax.fori_loop(1, S * T, greet, 0)
    small = [
        pltpu.make_async_copy(gain_h, norm_gain, in_sem.at[1]),
        pltpu.make_async_copy(head_gain_h, head_gain, in_sem.at[2]),
        pltpu.make_async_copy(lam_h, lam_all.at[t], in_sem.at[3]),
    ]
    for cp in small:
        cp.start()
    pairs = [(pk_h, pk), (pv_h, pv), (pq_h, pq), (wk_h, wk), (wv_h, wv), (wq_h, wq), (wg_h, wg), (pg_h, pg), (wo_h, wo), (po_h, po)]
    loads = [pltpu.make_async_copy(a, b, w_sem.at[i]) for i, (a, b) in enumerate(pairs)]
    with jax.named_scope("own_tok"):
        own_tok.wait()
        for cp in small:
            cp.wait()
    for cp in loads:
        cp.start()
    with jax.named_scope("barrier"):
        pl.semaphore_wait(barrier, S * T - 1)

    Rn = R // 2

    def tok_copy(dt, h):
        at = tok_buf.at[t, pl.ds(h * Rn, Rn)]
        return remote(at, at, tok_s.at[dt, h], tok_r.at[dt, h], dev(s, lax.rem(t + dt, T)))

    def tok_in(dt, h):
        at = tok_buf.at[lax.rem(t + T - dt, T), pl.ds(h * Rn, Rn)]
        return remote(at, at, tok_s.at[dt, h], tok_r.at[dt, h], dev(s, lax.rem(t + dt, T)))

    def lam_copy(dt):
        at = lam_all.at[t]
        return remote(at, at, lam_s.at[dt], lam_r.at[dt], dev(s, lax.rem(t + dt, T)))

    def lam_in(dt):
        at = lam_all.at[lax.rem(t + T - dt, T)]
        return remote(at, at, lam_s.at[dt], lam_r.at[dt], dev(s, lax.rem(t + dt, T)))

    for h in range(2):
        for dt in range(1, T):
            tok_copy(dt, h).start()
    for dt in range(1, T):
        lam_copy(dt).start()

    NB = 32

    def norm_rows(i, _):
        rows = pl.ds(pl.multiple_of(i * NB, NB), NB)
        xs = [tok_buf[k, rows, :].astype(F32) for k in range(T)]
        total = sum(jnp.sum(x * x, axis=-1, keepdims=True) for x in xs)
        r = lax.rsqrt(total * (1.0 / D) + norm_eps)
        for k in range(T):
            cols = slice(k * Dl, (k + 1) * Dl)
            normed[rows, cols] = (xs[k] * r * norm_gain[:, cols]).astype(BF16)
        return 0

    for h in range(2):
        with jax.named_scope(f"tok{h}"):
            for dt in range(1, T):
                tok_in(dt, h).wait_recv()
        with jax.named_scope(f"norm{h}"):
            lax.fori_loop(h * Rn // NB, (h + 1) * Rn // NB, norm_rows, 0, unroll=True)

    def project(i, store):
        loads[i].wait()
        w = pairs[i][1]
        cols = w.shape[1]
        tile = min(256, cols)
        for c in range(0, cols, tile):
            r = jnp.dot(normed[...], w[:, c : c + tile], preferred_element_type=F32).astype(BF16)
            store(c, tile, r)

    def by_head(put):
        def store(c, tile, r):
            for o in range(0, tile, C):
                put((c + o) // C, r[:, o : o + C])

        return store

    scale = HD**-0.5

    def put_k(j, r):
        k_send[j] = r

    def put_v(j, r):
        v_send[j] = r.T

    def put_q(j, r):
        q_send[j] = (r * scale).T

    def kv_copies(i, up, heads):
        src, dst = (k_send, k_all) if i == 0 else (v_send, v_all)
        out = []
        for j in heads:
            for p in range(PC):
                to = (j * T + t) * PC + p
                here = (up == 0) & (to == e) & (my_rc == t)
                base = E if up else half * E
                ss = kv_s.at[i, up, j * PC + p]
                out.append(Send(here, src.at[j], dst.at[up, e], ss, kv_r.at[i, up, e], dev(base + to, my_rc)))
        return out

    def q_copies(i, heads):
        out = []
        for j in heads:
            to = (j * T + t) * PC + my_p
            here = (i == 0) & (to == e) & (my_c == t)
            base = half * E if i == 0 else 0
            out.append(
                Send(here, q_send.at[j], q_all.at[i, my_k], q_s.at[i, j], q_r.at[i, my_k], dev(base + to, my_c))
            )
        return out

    n_relay = E // T

    def slot(i, up, n):
        return (k_all if i == 0 else v_all).at[up, n], kv_r.at[i, up, n]

    def relay_block(up, n, core):
        first = n_relay - 1 - n if up else lax.rem(e // T + n, n_relay)
        return first * T + core

    def relay_copy(i, up, n, dt):
        ref, rs = slot(i, up, relay_block(up, n, t))
        return remote(ref, ref, fw_s.at[i, up, n, dt], rs, dev(s, lax.rem(t + dt, T)))

    def relay(i, first, last, up=0):
        def one(n, _):
            ref, rs = slot(i, up, relay_block(up, n, t))
            arrived(ref, fw_s.at[i, up, n, 0], rs)
            for dt in range(1, T):
                relay_copy(i, up, n, dt).start()
            return 0

        with jax.named_scope(f"relay{i}{up}"):
            lax.fori_loop(first, last, one, 0)

    def peers(i, first, last, up=0):
        def one(n, _):
            core = lax.rem(t + 1 + lax.rem(n, T - 1), T)
            ref, rs = slot(i, up, relay_block(up, n // (T - 1), core))
            arrived(ref, fw_s.at[i, up, 0, 0], rs)
            return 0

        with jax.named_scope(f"peers{i}{up}"):
            lax.fori_loop(first * (T - 1), last * (T - 1), one, 0)

    def begin(copies):
        for cp in copies:
            cp.start()

    def begin(copies):
        for cp in copies:
            cp.start()

    high = jnp.logical_not(low)

    with jax.named_scope("proj_k"):
        project(0, by_head(put_k))

        @pl.when(high)
        def _():
            begin(kv_copies(0, 0, downs + ups))

        @pl.when(low)
        def _():
            begin(kv_copies(0, 0, downs))

    with jax.named_scope("proj_v"):
        project(1, by_head(put_v))

        @pl.when(low)
        def _():
            begin(kv_copies(1, 0, downs))
            for i in range(2):
                begin(kv_copies(i, 1, ups))

    with jax.named_scope("proj_q"):
        project(2, by_head(put_q))

        @pl.when(high)
        def _():
            begin(q_copies(0, downs + ups))
            begin(q_copies(1, downs[::-1]))
            begin(kv_copies(1, 0, ups))

    def late_low():
        for i in range(2):
            begin(kv_copies(i, 0, ups))
        begin(q_copies(0, ups + downs))

    def late_high():
        begin(kv_copies(1, 0, downs))

    def into(ref, first=0):
        def store(c, tile, r):
            ref[first:, c : c + tile] = r

        return store

    with jax.named_scope("proj_band"):
        project(3, into(band_k, WINDOW))
        project(4, into(band_v, WINDOW))

    def tails():
        return [
            remote(
                b.at[pl.ds(R, WINDOW)], b.at[pl.ds(0, WINDOW)], tail_s.at[i], tail_r.at[i], dev(lax.rem(s + 1, S), t)
            )
            for i, b in enumerate((band_k, band_v))
        ]

    @pl.when(s < S - 1)
    def _():
        for cp in tails():
            cp.start()

    @pl.when(s == 0)
    def _():
        band_k[0:WINDOW] = jnp.zeros((WINDOW, band_k.shape[1]), BF16)
        band_v[0:WINDOW] = jnp.zeros((WINDOW, band_v.shape[1]), BF16)

    with jax.named_scope("proj_sq"):
        project(5, into(sq_buf))
    with jax.named_scope("proj_sg"):
        project(6, into(sg_buf))
    with jax.named_scope("proj_pg"):
        project(7, into(pg_buf))

    kv_heads = band_k.shape[1] // HD
    group = sq_buf.shape[1] // band_k.shape[1]
    W = WINDOW
    blocks = R // W
    key_i = lax.broadcasted_iota(jnp.int32, (2 * W, group * W), 0)
    qry_i = lax.rem(lax.broadcasted_iota(jnp.int32, (2 * W, group * W), 1), W)
    lane_head = lax.broadcasted_iota(jnp.int32, (1, group * W), 1) // W
    dist = qry_i - key_i + W
    in_band = (dist >= 0) & (dist < W)

    def window_block(b):
        r0 = b * W
        ok = in_band & (s * R + r0 - W + key_i >= 0)
        for h in range(kv_heads):
            k = band_k[r0 : r0 + 2 * W, h * HD : (h + 1) * HD]
            v = band_v[r0 : r0 + 2 * W, h * HD : (h + 1) * HD]
            q = jnp.concatenate(
                [sq_buf[r0 : r0 + W, (h * group + g) * HD : (h * group + g + 1) * HD] for g in range(group)], axis=0
            )
            sc = jnp.where(ok, dot_nt(k, q) * scale, -jnp.inf)
            sk = jnp.full((1, group * W), sink[0, h * group], F32)
            for g in range(1, group):
                sk = jnp.where(lane_head == g, sink[0, h * group + g], sk)
            top = jnp.maximum(jnp.max(sc, axis=0, keepdims=True), sk)
            w = jnp.exp(sc - top)
            den = jnp.sum(w, axis=0, keepdims=True) + jnp.exp(sk - top)
            probs = (w * (1.0 / den)).astype(BF16)
            o = dot_tn(v, probs)
            o = jnp.concatenate([o[:, g * W : (g + 1) * W] for g in range(group)], axis=0).T
            cols = slice(h * group * HD, (h + 1) * group * HD)
            gate = sg_buf[r0 : r0 + W, cols].astype(F32)
            slide_mix[r0 : r0 + W, cols] = (o * silu(gate)).astype(BF16)

    def other_windows():
        for b in range(1, blocks):
            with jax.named_scope(f"win{b}"):
                window_block(b)

    pl.when(low)(other_windows)
    relay(0, 0, n_relay)
    peers(0, 0, n_relay)

    def queries():
        with jax.named_scope("q_wait"):
            for k in range(KB):
                arrived(q_all.at[0, k], q_s.at[0, 0], q_r.at[0, k])

    pl.when(jnp.logical_not(low))(queries)
    row = lax.broadcasted_iota(jnp.int32, (C, R), 0)
    ones = jnp.ones((ONES, R), BF16)

    def scores(q, up, bs, first_masked, mine):
        zero = jnp.zeros_like(q)
        q2 = jnp.concatenate([jnp.where(row < HD, q, zero), jnp.where(row < HD, zero, q)], axis=1)
        top8 = None
        for i, b in enumerate(bs):
            st = jnp.dot(k_all[up, b], q2, preferred_element_type=F32)
            if b >= first_masked:
                ki = lax.broadcasted_iota(jnp.int32, (R, 2 * R), 0)
                qi = lax.rem(lax.broadcasted_iota(jnp.int32, (R, 2 * R), 1), R)
                st = jnp.where(qi - ki >= (b - mine) * R, st, -jnp.inf)
            s_buf[i] = st
            m8 = jnp.max(st.reshape(R // 8, 8, 2 * R), axis=0)
            top8 = m8 if top8 is None else jnp.maximum(top8, m8)
        return jnp.max(top8, axis=0, keepdims=True)

    def chunks_of(n):
        return [range(f, min(n, f + CHUNK)) for f in range(0, n, CHUNK)]

    def stats(k):
        total = top = None
        for bs in chunks_of(NQ * (k + 1)):
            old = top
            top = scores(q_all[0, k], 0, bs, NQ * k, block(k))
            if old is not None:
                top = jnp.maximum(top, old)
                total = total * jnp.exp(old - top)
            for i in range(len(bs)):
                p = jnp.sum(jnp.exp(s_buf[i] - top).reshape(R // 8, 8, 2 * R), axis=0)
                total = p if total is None else total + p
        stat_send[2 * k] = top
        stat_send[2 * k + 1] = jnp.sum(total, axis=0, keepdims=True)

    other = dev((1 - half) * E + e, t)

    def stat_copy():
        return remote(stat_send, stat_in, stat_s, stat_r, other)

    @pl.when(asking_core)
    def _():
        with jax.named_scope("stats"):
            for k in range(KB):
                stats(k)
            stat_copy().start()

    pl.when(high)(late_high)
    pl.when(high)(other_windows)

    def values():
        relay(1, 0, n_relay)
        peers(1, 0, n_relay)

    pl.when(jnp.logical_not(up_core))(values)
    pl.when(low)(late_low)

    for dt in range(1, T):
        lam_in(dt).wait_recv()
    lam_lane = lax.broadcasted_iota(jnp.int32, (1, H), 1)
    lam = jnp.sum(jnp.where(lam_lane == jh, lam_all[th], 0.0), axis=1, keepdims=True)

    def attend(q, up, parts, first_masked, mine, acc_ref, top_ref, fresh):
        for bs in parts:
            top = scores(q, up, bs, first_masked, mine)
            if not fresh:
                old = top_ref[...]
                top = jnp.maximum(top, old)
            for i in range(len(bs)):
                p_buf[i] = jnp.exp(s_buf[i] - top).astype(BF16)
            v = jnp.concatenate([v_all[up, b] for b in bs], axis=1)
            v = jnp.concatenate([v, jnp.concatenate([ones] * len(bs), axis=1)], axis=0)
            acc = jnp.dot(v, p_buf[0 : len(bs)].reshape(len(bs) * R, 2 * R), preferred_element_type=F32)
            if not fresh:
                acc = acc + acc_ref[...] * jnp.exp(old - top)
            acc_ref[...] = acc
            top_ref[...] = top
            fresh = False

    def own_block(k):
        with jax.named_scope(f"own{k}"):
            attend(q_all[0, k], 0, chunks_of(NQ * (k + 1)), NQ * k, block(k), own_acc.at[k], own_top.at[k], False)

    def down_block(k, _):
        with jax.named_scope("down"):
            arrived(q_all.at[1, k], q_s.at[1, 0], q_r.at[1, k])
            attend(q_all[1, k], 0, chunks_of(E), E, 0, up_acc.at[k], up_top.at[k], True)
        return 0

    def upper(parts, fresh, last):
        def one(k, _):
            with jax.named_scope("upper"):
                attend(q_all[0, k], 1, parts, E, 0, own_acc.at[k], own_top.at[k], fresh)
                if last:
                    finish_low(k)
            return 0

        lax.fori_loop(0, KB, one, 0)

    def share_copy(k):
        return remote(share_send.at[k], share_in.at[k], share_s.at[k], share_r.at[k], other)

    def coef_copy(k):
        return remote(coef_send.at[k], coef_in.at[k], coef_s.at[k], coef_r.at[k], other)

    def share_block(k, _):
        with jax.named_scope("share"):
            top = up_top[k]
            far_top = stat_in[2 * k]
            both = jnp.maximum(top, far_top)
            f = jnp.exp(top - both)
            far_f = jnp.exp(far_top - both)
            inv = 1.0 / (up_acc[k, C : C + 1] * f + stat_in[2 * k + 1] * far_f)
            coef_send[k] = far_f * inv
            a = up_acc[k, 0:C] * (f * inv)
            share_send[k] = (a[:, 0:R] - lam * a[:, R:]).astype(BF16)
            coef_copy(k).start()
            share_copy(k).start()
        return 0

    def ret_copy(k):
        b = block(k)
        here = (b == e) & (th == t)
        return Send(here, ret_send.at[k], ret_all.at[jh], ret_s.at[k], ret_r.at[jh], dev(half * E + b, th))

    def give_back(k, d):
        sq = jnp.mean(d * d, axis=0, keepdims=True)
        y = (d * (lax.rsqrt(sq + norm_eps) * head_scale)).T * head_gain[...]
        ret_send[k] = y.astype(BF16)
        ret_copy(k).start()

    def finish_low(k):
        with jax.named_scope("fin"):
            a = own_acc[k, 0:C] * (1.0 / own_acc[k, C : C + 1])
            give_back(k, a[:, 0:R] - lam * a[:, R:])

    def finish_high(k):
        with jax.named_scope(f"share_wait{k}"):
            arrived(coef_in.at[k], coef_s.at[k], coef_r.at[k])
            arrived(share_in.at[k], share_s.at[k], share_r.at[k])
        a = own_acc[k, 0:C] * coef_in[k]
        give_back(k, a[:, 0:R] - lam * a[:, R:] + share_in[k].astype(F32))

    @pl.when(down_core)
    def _():
        ready = 1
        lax.fori_loop(0, ready, down_block, 0)
        with jax.named_scope("stat_wait"):
            arrived(stat_in, stat_s, stat_r)
        lax.fori_loop(0, ready, share_block, 0)
        for k in range(ready, KB):
            down_block(k, 0)
            share_block(k, 0)

    pl.when(low)(queries)
    @pl.when(jnp.logical_not(up_core))
    def _():
        own_acc[...] = jnp.zeros(own_acc.shape, F32)
        own_top[...] = jnp.full(own_top.shape, -1e30, F32)

    NT = min(512, D)

    def first_window():
        with jax.named_scope("tail"):

            @pl.when(s > 0)
            def _():
                for cp in tails():
                    cp.wait_recv()

        with jax.named_scope("win0"):
            window_block(0)
        with jax.named_scope("wo"):
            loads[8].wait()
            for c in range(0, D, NT):
                part[:, c : c + NT] = jnp.dot(slide_mix[...], wo[:, c : c + NT], preferred_element_type=F32)

    n_near = n_relay // 2
    near, far = range((n_relay - n_near) * T, E), range(0, (n_relay - n_near) * T)
    if ups:

        @pl.when(up_core)
        def _():
            for i in range(2):
                relay(i, 0, n_near, 1)
            for i in range(2):
                peers(i, 0, n_near, 1)
            upper([near], True, False)
            first_window()
            values()

    for k in range(KB):
        if k == KB // 2 and ups:

            @pl.when(up_core)
            def _():
                for i in range(2):
                    relay(i, n_near, n_relay, 1)

        own_block(k)

        @pl.when(low)
        def _(k=k):
            finish_low(k)

    if ups:

        @pl.when(up_core)
        def _():
            for i in range(2):
                peers(i, n_near, n_relay, 1)
            upper([far], False, True)

    pl.when(jnp.logical_not(up_core))(first_window)

    @pl.when(asking_core)
    def _():
        for k in range(KB):
            finish_high(k)

    gate = pg_buf[...].astype(F32)
    gate_buf[...] = silu(gate)
    def gated(heads):
        with jax.named_scope("ret_wait"):
            for j in heads:
                arrived(ret_all.at[j], ret_s.at[0], ret_r.at[j])
        for j in heads:
            cols = slice(j * C, (j + 1) * C)
            paired_mix[:, cols] = (ret_all[j].astype(F32) * gate_buf[:, cols]).astype(BF16)

    loads[9].wait()
    H1 = H // 2
    if H1:
        gated(range(H1))
        for c in range(0, D, NT):
            part[:, c : c + NT] += jnp.dot(
                paired_mix[:, 0 : H1 * C], po[0 : H1 * C, c : c + NT], preferred_element_type=F32
            )
    gated(range(H1, H))
    Rt = R // T
    chunks = range(0, D, NT)

    def rs_copy(dt, i):
        cols = pl.ds(i * NT, NT)
        return remote(
            part_bf.at[lax.rem(t + dt, T), :, cols],
            out_in.at[dt - 1, :, cols],
            rs_s.at[dt, i],
            rs_r.at[dt, i],
            dev(s, lax.rem(t + dt, T)),
        )

    def own_out(i):
        cols = pl.ds(i * NT, NT)
        return pltpu.make_async_copy(part_bf.at[t, :, cols], out_own.at[:, cols], rs_s.at[0, i])

    with jax.named_scope("po"):
        for i, c in enumerate(chunks):
            r = part[:, c : c + NT] + jnp.dot(
                paired_mix[:, H1 * C :], po[H1 * C :, c : c + NT], preferred_element_type=F32
            )
            r = r.astype(BF16)
            for k in range(T):
                part_bf[k, :, c : c + NT] = r[k * Rt : (k + 1) * Rt]
            for dt in range(1, T):
                rs_copy(dt, i).start()
            own_out(i).start()

    with jax.named_scope("drain"):
        for h in range(2):
            for dt in range(1, T):
                tok_copy(dt, h).wait_send()
        for dt in range(1, T):
            lam_copy(dt).wait_send()
        def relayed(up):
            def one(n, _):
                for i in range(2):
                    for dt in range(1, T):
                        relay_copy(i, up, n, dt).wait_send()
                return 0

            lax.fori_loop(0, n_relay, one, 0)

        relayed(0)
        for i in range(2):
            for cp in kv_copies(i, 0, range(H)):
                cp.wait_send()
        for cp in q_copies(0, range(H)):
            cp.wait_send()

        @pl.when(half == 1)
        def _():
            for cp in q_copies(1, downs):
                cp.wait_send()

        @pl.when(low)
        def _():
            for i in range(2):
                for cp in kv_copies(i, 1, ups):
                    cp.wait_send()

        if ups:
            pl.when(up_core)(lambda: relayed(1))

        @pl.when(asking_core)
        def _():
            stat_copy().wait_send()

        @pl.when(down_core)
        def _():
            for k in range(KB):
                coef_copy(k).wait_send()
                share_copy(k).wait_send()

        for k in range(KB):
            ret_copy(k).wait_send()

        @pl.when(s < S - 1)
        def _():
            for cp in tails():
                cp.wait_send()

    with jax.named_scope("rs_wait"):
        for i in range(D // NT):
            own_out(i).wait()
            for dt in range(1, T):
                rs_copy(dt, i).wait_send()
                rs_copy(dt, i).wait_recv()


def per_device(S, T, tokens, norm_gain, wq, wk, wv, wg, sink, pq, pk, pv, pg, lam, head_gain, wo, po):
    R, Dl = tokens.shape
    D = Dl * T
    A = wq.shape[1]
    KC = wk.shape[1]
    B = pq.shape[1]
    C = 2 * HD
    H = B // C
    E = S // 2
    PC = E // (H * T)
    KB = E // (PC * T)
    if S % 2 or PC * H * T != E:
        raise ValueError("unsupported mesh")
    Rt = R // T
    NC = D // min(512, D)
    smem = pl.BlockSpec(memory_space=pltpu.SMEM)
    hbm = pl.BlockSpec(memory_space=pl.ANY)
    dma = pltpu.SemaphoreType.DMA
    V = pltpu.VMEM
    scratch = [V(w.shape, BF16) for w in (wq, wk, wv, wg, pq, pk, pv, pg, wo, po)]
    scratch += [
        V((1, D), F32),
        V((1, C), F32),
        V((T, 1, H), F32),
        V((T, R, Dl), BF16),
        V((R, D), BF16),
        V((WINDOW + R, KC), BF16),
        V((WINDOW + R, KC), BF16),
        V((R, A), BF16),
        V((R, A), BF16),
        V((R, B), BF16),
        V((R, B), F32),
        V((R, A), BF16),
        V((R, B), BF16),
        V((H, R, C), BF16),
        V((H, C, R), BF16),
        V((H, C, R), BF16),
        V((2, E, R, C), BF16),
        V((2, E, C, R), BF16),
        V((2, KB, C, R), BF16),
        V((min(E, CHUNK), R, 2 * R), F32),
        V((min(E, CHUNK), R, 2 * R), BF16),
        V((KB, C + ONES, 2 * R), F32),
        V((KB, 1, 2 * R), F32),
        V((KB, C + ONES, 2 * R), F32),
        V((KB, 1, 2 * R), F32),
        V((2 * KB, 1, 2 * R), F32),
        V((2 * KB, 1, 2 * R), F32),
        V((KB, C, R), BF16),
        V((KB, C, R), BF16),
        V((KB, 1, 2 * R), F32),
        V((KB, 1, 2 * R), F32),
        V((KB, R, C), BF16),
        V((H, R, C), BF16),
        V((R, D), F32),
        V((T, Rt, D), BF16),
        dma((10,)),
        dma((4,)),
        dma((T, 2)),
        dma((T, 2)),
        dma((T,)),
        dma((T,)),
        dma((2, 2, H * PC)),
        dma((2, 2, E // T, T)),
        dma((2, 2, E)),
        dma((2, H)),
        dma((2, KB)),
        dma((2,)),
        dma((2,)),
        dma,
        dma,
        dma((KB,)),
        dma((KB,)),
        dma((KB,)),
        dma((KB,)),
        dma((KB,)),
        dma((H,)),
        dma((T, NC)),
        dma((T, NC)),
    ]
    own, others = pl.pallas_call(
        functools.partial(kernel, S, T),
        out_shape=[jax.ShapeDtypeStruct((Rt, D), BF16), jax.ShapeDtypeStruct((T - 1, Rt, D), BF16)],
        in_specs=[hbm, hbm, hbm, hbm, hbm, hbm, smem, hbm, hbm, hbm, hbm, hbm, hbm, hbm, hbm],
        out_specs=[hbm, hbm],
        scratch_shapes=scratch,
        compiler_params=pltpu.CompilerParams(
            collective_id=0, has_side_effects=True, vmem_limit_bytes=60 * 1024 * 1024
        ),
        name="layer",
    )(
        tokens,
        norm_gain.reshape(1, D),
        wq,
        wk,
        wv,
        wg,
        sink.reshape(1, -1),
        pq,
        pk,
        pv,
        pg,
        lam.reshape(1, -1),
        head_gain.reshape(1, -1),
        wo,
        po,
    )
    return (own.astype(F32) + jnp.sum(others.astype(F32), axis=0)).astype(BF16)


def solution(mesh):
    S, T = mesh.shape["sp"], mesh.shape["tp"]
    in_specs = (
        P("sp", "tp"),
        P(),
        P(None, "tp"),
        P(None, "tp"),
        P(None, "tp"),
        P(None, "tp"),
        P("tp"),
        P(None, "tp"),
        P(None, "tp"),
        P(None, "tp"),
        P(None, "tp"),
        P("tp"),
        P(),
        P("tp", None),
        P("tp", None),
    )
    return jax.shard_map(
        functools.partial(per_device, S, T),
        mesh=mesh,
        in_specs=in_specs,
        out_specs=P(("sp", "tp"), None),
        check_vma=False,
    )
```
